32 devices in a mesh: fs: 8 (over z, core), tp: 4 (over y, x).
Axes of the slice: x: 2, y: 2, z: 4, core: 2. Of those that a mesh axis runs over, the one named last changes fastest.
Arguments:
- latent: bfloat16 [16384, 1024], P('fs'), may hold values from -6 to 6
- key_cotangent: bfloat16 [16384, 512], P('fs', 'tp'), may hold values from -0.046875 to 0.046875
- value_cotangent: bfloat16 [16384, 512], P('fs', 'tp'), may hold values from -0.046875 to 0.046875
- key_weight: float32 [1024, 512], P('fs', 'tp'), may hold values from -50 to 50
- value_weight: float32 [1024, 512], P('fs', 'tp'), may hold values from -50 to 50
- key_projector: bfloat16 [1024, 256], replicated, may hold values from -0.1875 to 0.1875
- value_projector: bfloat16 [1024, 256], replicated, may hold values from -0.1875 to 0.1875
- key_first: float32 [256, 512], P(None, 'tp'), may hold values from -6 to 6
- key_second: float32 [256, 512], P(None, 'tp'), may hold values from 0.3 to 3
- value_first: float32 [256, 512], P(None, 'tp'), may hold values from -6 to 6
- value_second: float32 [256, 512], P(None, 'tp'), may hold values from 0.3 to 3
Outputs:
- key_renewed: float32 [1024, 512], P('fs', 'tp')
- value_renewed: float32 [1024, 512], P('fs', 'tp')
- key_step: float32 [1024, 512], P('fs', 'tp')
- value_step: float32 [1024, 512], P('fs', 'tp')
- key_first_new: float32 [256, 512], P(None, 'tp')
- key_second_new: float32 [256, 512], P(None, 'tp')
- value_first_new: float32 [256, 512], P(None, 'tp')
- value_second_new: float32 [256, 512], P(None, 'tp')
- key_copy: bfloat16 [1024, 512], P(None, 'tp')
- value_copy: bfloat16 [1024, 512], P(None, 'tp')
The draws below stay inside these ranges and needn't reach their ends.
All inputs are finite; a program needn't handle non-finite values.
Results may differ from the reference program's by a relative error of at most 0.015.
Values may be sent and summed in bfloat16 or wider, within the bound.
A program may use at most 64 MiB of HBM per device.

```python
import math
import jax
import jax.numpy as jnp
from jax import lax

LATENT_WIDTH = 1024
KEY_FEATURES = 128
VALUE_FEATURES = 128
FACTOR_RANK = 256
ATTENTION_HEADS = 4
TOKEN_COUNT = 16384
KEY_COLS = 512
VALUE_COLS = 512


def draw_weight_common(key, row_total, col_total):
    row_place = jnp.arange(row_total, dtype=jnp.float32) / row_total
    col_place = jnp.arange(col_total, dtype=jnp.float32) / col_total
    keys = jax.random.split(key, 3)
    row_scale = 10.0 ** row_place
    col_scale = 10.0 ** col_place
    values = jnp.clip(jax.random.normal(keys[2], (row_total, col_total), jnp.float32), -5.0, 5.0)
    return (values * jnp.sqrt(row_scale[:, None] * col_scale[None, :])).astype(jnp.float32)


def draw_key_weight(key, part):
    return draw_weight_common(jax.random.fold_in(key, 11), LATENT_WIDTH, ATTENTION_HEADS * KEY_FEATURES)


def draw_value_weight(key, part):
    return draw_weight_common(jax.random.fold_in(key, 23), LATENT_WIDTH, ATTENTION_HEADS * VALUE_FEATURES)


def strengthened(entries, key, source, target, shards_of, factor):
    owner, partner = [(jnp.arange(entries.shape[position]) // (entries.shape[position] // shards_of)).reshape([-1 if axis == position else 1 for axis in range(entries.ndim)]) for position in (source, target)]
    chosen = jax.random.permutation(key, shards_of)[partner]
    strong = (owner == chosen) | (owner == (partner + shards_of // 2) % shards_of)
    return jnp.where(strong, factor * entries, entries)


def levels(rng, extent, shards, smallest, top_value):
    gain, own = 1.0, jax.random.fold_in(rng, 6)
    for axis_at, parts in shards:
        heights = jnp.exp(jax.random.uniform(jax.random.fold_in(own, axis_at), (parts,), jnp.float32, smallest / len(shards), top_value / len(shards)))
        gain = gain * jnp.repeat(heights, extent[axis_at] // parts).reshape([-1 if axis == axis_at else 1 for axis in range(len(extent))])
    return gain


def noise(stream_key, shape, spread, reach, cuts=(), kind=jnp.bfloat16):
    entries = jax.random.normal(stream_key, shape, jnp.float32) * spread
    if len(cuts) > 0:
        entries = levels(stream_key, shape, cuts, -0.22, 0.18) * entries
    return jnp.clip(entries, min=-reach, max=reach).astype(kind)


def heavy_noise(own_key, extent, scale, most, pieces, heavy, held_as=jnp.bfloat16):
    array = scale * jax.random.normal(own_key, extent, jnp.float32)
    if pieces:
        array = array * levels(own_key, extent, pieces, -0.22, 0.18)
    return jnp.clip(strengthened(array, jax.random.fold_in(own_key, 3), *heavy), -most, most).astype(held_as)


def setup_inputs(seed: int = 0) -> dict:
    splits = jax.random.split(jax.random.key(seed), 12)
    return {
        "latent": heavy_noise(splits[0], (TOKEN_COUNT, LATENT_WIDTH), 1.0, 6.0, ((0, 8),), (0, 1, 8, 2.0)),
        "key_cotangent": noise(splits[1], (TOKEN_COUNT, KEY_COLS), (1.0 / TOKEN_COUNT ** 0.5), 0.046875, ((0, 8), (1, 4))),
        "value_cotangent": noise(splits[2], (TOKEN_COUNT, VALUE_COLS), (1.0 / TOKEN_COUNT ** 0.5), 0.046875, ((0, 8), (1, 4))),
        "key_weight": draw_key_weight(jax.random.fold_in(splits[11], 71), 0),
        "value_weight": draw_value_weight(jax.random.fold_in(splits[11], 71), 0),
        "key_projector": noise(splits[5], (LATENT_WIDTH, FACTOR_RANK), LATENT_WIDTH ** -0.5, 0.1875),
        "value_projector": noise(splits[6], (LATENT_WIDTH, FACTOR_RANK), LATENT_WIDTH ** -0.5, 0.1875),
        "key_first": noise(splits[7], (FACTOR_RANK, KEY_COLS), 1.0, 6.0, ((1, 4),), jnp.float32),
        "key_second": jnp.clip(jnp.exp(math.log(3.0) - 2.3025851 * jax.random.uniform(splits[8], (FACTOR_RANK, KEY_COLS), jnp.float32) ** levels(splits[8], (FACTOR_RANK, KEY_COLS), ((1, 4),), -0.2, 0.2)), 0.3, 3.0),
        "value_first": noise(splits[9], (FACTOR_RANK, VALUE_COLS), 1.0, 6.0, ((1, 4),), jnp.float32),
        "value_second": jnp.clip(jnp.exp(math.log(3.0) - 2.3025851 * jax.random.uniform(splits[10], (FACTOR_RANK, VALUE_COLS), jnp.float32) ** levels(splits[10], (FACTOR_RANK, VALUE_COLS), ((1, 4),), -0.2, 0.2)), 0.3, 3.0),
    }


EPSILON = 1e-08
FIRST_DECAY = 0.7
SECOND_DECAY = 0.8
LEARN_RATE = 0.2

def update(latent, weight, factor, cotangent, first_moment, second):
    reduced = jnp.dot(latent.astype(jnp.float32), factor.astype(jnp.float32), precision=lax.Precision.HIGHEST)
    projected = jnp.dot(reduced.T, cotangent.astype(jnp.float32), precision=lax.Precision.HIGHEST)
    first_new = FIRST_DECAY * first_moment + (1.0 - FIRST_DECAY) * projected
    second_new = SECOND_DECAY * second + (1.0 - SECOND_DECAY) * projected * projected
    normalized = first_new / (jnp.sqrt(second_new) + EPSILON)
    direction = jnp.dot(factor.astype(jnp.float32), normalized, precision=lax.Precision.HIGHEST)
    step_scale = LEARN_RATE * jnp.sqrt(jnp.mean(weight * weight))
    weight_step = step_scale * direction
    renewed = weight - weight_step
    return (renewed, weight_step, first_new, second_new, renewed.astype(jnp.bfloat16))

def reference(latent, key_cotangent, value_cotangent, key_weight, value_weight, key_projector, value_projector, key_first, key_second, value_first, value_second):
    key_out = update(latent, key_weight, key_projector, key_cotangent, key_first, key_second)
    value_out = update(latent, value_weight, value_projector, value_cotangent, value_first, value_second)
    return (key_out[0], value_out[0], key_out[1], value_out[1], key_out[2], key_out[3], value_out[2], value_out[3], key_out[4], value_out[4])
```

```python
import functools

import jax
import jax.numpy as jnp
from jax import lax
from jax.experimental import pallas as pl
from jax.experimental.pallas import tpu as pltpu
from jax.sharding import PartitionSpec as P

EPSILON = 1e-08
FIRST_DECAY = 0.7
SECOND_DECAY = 0.8
LEARN_RATE = 0.2
CHUNKS = 4
MESH = pl.DeviceIdType.MESH
HBM = pl.BlockSpec(memory_space=pltpu.MemorySpace.HBM)
VMEM = pl.BlockSpec(memory_space=pltpu.MemorySpace.VMEM)


def exchange_kernel(
    n,
    m,
    latent,
    key_cot,
    value_cot,
    key_weight,
    value_weight,
    key_proj,
    value_proj,
    gathered,
    weights,
    squares,
    latent_v,
    cot_v,
    cot_t,
    weight_v,
    proj_v,
    partial,
    received,
    tp_squares,
    load_sem,
    latent_sem,
    rs_send,
    rs_recv,
    ag_send,
    ag_recv,
    w_send,
    w_recv,
    f_send,
    f_recv,
    t_send,
    t_recv,
    s_send,
    s_recv,
):
    me = lax.axis_index("fs")
    mine = lax.axis_index("tp")
    core = lax.rem(me, 2)
    partner = me + 1 - 2 * core
    half = n // 2
    tokens, width = latent.shape
    step = width // CHUNKS
    rank = key_proj.shape[1]
    cols = key_cot.shape[1]
    piece = partial.shape[0] // n
    f32, bf16 = jnp.float32, jnp.bfloat16

    loads = [
        pltpu.make_async_copy(src, dst, load_sem.at[i])
        for i, (src, dst) in enumerate(
            (
                (key_weight, weight_v.at[0]),
                (value_weight, weight_v.at[1]),
                (key_cot, cot_v.at[0]),
                (value_cot, cot_v.at[1]),
                (key_proj, proj_v.at[0]),
                (value_proj, proj_v.at[1]),
            )
        )
    ]
    streams = [
        pltpu.make_async_copy(
            latent.at[:, pl.ds(c * step, step)], latent_v.at[c], latent_sem.at[c]
        )
        for c in range(CHUNKS)
    ]
    for copy in loads[:4]:
        copy.start()
    streams[0].start()
    for copy in loads[4:]:
        copy.start()
    for copy in streams[1:]:
        copy.start()

    barrier = pltpu.get_barrier_semaphore()
    for d in range(1, n):
        pl.semaphore_signal(
            barrier, inc=1, device_id={"fs": lax.rem(me + d, n)}, device_id_type=MESH
        )
    for d in range(1, m):
        pl.semaphore_signal(
            barrier, inc=1, device_id={"tp": lax.rem(mine + d, m)}, device_id_type=MESH
        )

    def send(src, dst, send_sem, recv_sem, where):
        copy = pltpu.make_async_remote_copy(
            src_ref=src,
            dst_ref=dst,
            send_sem=send_sem,
            recv_sem=recv_sem,
            device_id=where,
            device_id_type=MESH,
        )
        copy.start()
        return copy

    def arrived(ref, sem):
        pltpu.make_async_remote_copy(
            src_ref=ref,
            dst_ref=ref,
            send_sem=sem,
            recv_sem=sem,
            device_id={"fs": partner},
            device_id_type=MESH,
        ).wait_recv()

    sent = []
    loads[0].wait()
    loads[1].wait()
    for i in range(2):
        w = weight_v[i]
        weights[me, i] = w.astype(bf16)
        tp_squares[mine, pl.ds(8 * i, 8), :] = jnp.sum(
            (w * w).reshape(w.shape[0] // 8, 8, w.shape[1]), axis=0
        )
    loads[2].wait()
    loads[3].wait()
    for i in range(2):
        cot_t[pl.ds(i * cols, cols), :] = cot_v[i].T

    pl.semaphore_wait(barrier, n - 1 + m - 1)

    def send_weights(d):
        sent.append(
            send(
                weights.at[me],
                weights.at[me],
                w_send.at[d],
                w_recv.at[me],
                {"fs": lax.rem(me + 2 * d, n)},
            )
        )

    for d in range(1, m):
        sent.append(
            send(
                tp_squares.at[mine],
                tp_squares.at[mine],
                t_send.at[d],
                t_recv.at[mine],
                {"tp": lax.rem(mine + d, m)},
            )
        )
    sent.append(
        send(
            weights.at[me], weights.at[me], f_send.at[0], f_recv.at[me], {"fs": partner}
        )
    )
    for d in range(1, half):
        send_weights(d)

    totals = [None, None]
    for c in range(CHUNKS):
        streams[c].wait()
        g = jnp.dot(cot_t[...], latent_v[c], preferred_element_type=f32).astype(bf16)
        if c == 0:
            loads[4].wait()
            loads[5].wait()
        for i in range(2):
            term = jnp.dot(
                g[i * cols : (i + 1) * cols],
                proj_v[i, pl.ds(c * step, step), :],
                preferred_element_type=f32,
            )
            totals[i] = term if totals[i] is None else totals[i] + term
    for i in range(2):
        partial[pl.ds(i * rank, rank), :] = totals[i].T.astype(bf16)

    for d in range(1, m):
        arrived(tp_squares.at[lax.rem(mine + d, m)], t_recv.at[lax.rem(mine + d, m)])
    squares[me] = jnp.sum(tp_squares[...], axis=0)

    for d in range(n - 1, 0, -1):
        peer = lax.rem(me + d, n)
        sent.append(
            send(
                partial.at[pl.ds(peer * piece, piece)],
                received.at[me],
                rs_send.at[d],
                rs_recv.at[me],
                {"fs": peer},
            )
        )
    received[me] = partial[pl.ds(pl.multiple_of(me * piece, piece), piece), :]
    for d in range(1, n):
        sent.append(
            send(
                squares.at[me],
                squares.at[me],
                s_send.at[d],
                s_recv.at[me],
                {"fs": lax.rem(me + d, n)},
            )
        )
    for d in range(1, n):
        peer = lax.rem(me + d, n)
        arrived(received.at[peer], rs_recv.at[peer])
    gathered[me] = jnp.sum(received[...].astype(f32), axis=0).astype(bf16)
    for d in range(n - 1, 0, -1):
        sent.append(
            send(
                gathered.at[me],
                gathered.at[me],
                ag_send.at[d],
                ag_recv.at[me],
                {"fs": lax.rem(me + d, n)},
            )
        )
    for d in range(1, half):
        source = lax.rem(me + 2 * d, n)
        arrived(weights.at[source], w_recv.at[source])
        sent.append(
            send(
                weights.at[source],
                weights.at[source],
                f_send.at[d],
                f_recv.at[source],
                {"fs": partner},
            )
        )
    for d in range(half):
        source = lax.rem(partner + 2 * d, n)
        arrived(weights.at[source], f_recv.at[source])
    for d in range(1, n):
        peer = lax.rem(me + d, n)
        arrived(squares.at[peer], s_recv.at[peer])
    for d in range(1, n):
        peer = lax.rem(me + d, n)
        arrived(gathered.at[peer], ag_recv.at[peer])
    for copy in sent:
        copy.wait_send()


def update_kernel(n, entries, *refs):
    (
        gathered,
        weights,
        squares,
        key_weight,
        value_weight,
        key_proj,
        value_proj,
        key_first,
        key_second,
        value_first,
        value_second,
    ) = refs[:11]
    outs = refs[11:]
    me = lax.axis_index("fs")
    f32, bf16 = jnp.float32, jnp.bfloat16
    parts = n // 2
    tile = jnp.sum(squares[...], axis=0)
    for i, (weight, proj, first, second) in enumerate(
        (
            (key_weight, key_proj, key_first, key_second),
            (value_weight, value_proj, value_first, value_second),
        )
    ):
        rows = weight.shape[0]
        rank, cols = first.shape
        projected = (
            gathered[i * parts : (i + 1) * parts].astype(f32).reshape(rank, cols)
        )
        first_new = FIRST_DECAY * first[...] + (1.0 - FIRST_DECAY) * projected
        second_new = (
            SECOND_DECAY * second[...] + (1.0 - SECOND_DECAY) * projected * projected
        )
        outs[4 + 2 * i][...] = first_new
        outs[5 + 2 * i][...] = second_new
        normalized = (first_new / (jnp.sqrt(second_new) + EPSILON)).astype(bf16)
        total = jnp.sum(tile[8 * i : 8 * i + 8], keepdims=True)
        scale = LEARN_RATE * jnp.sqrt(total / entries)
        own = proj[pl.ds(pl.multiple_of(me * rows, rows), rows), :]
        own_step = scale * jnp.dot(own, normalized, preferred_element_type=f32)
        outs[2 + i][...] = own_step
        outs[i][...] = weight[...] - own_step
        every = scale * jnp.dot(proj[...], normalized, preferred_element_type=f32)
        held = weights[:, i].astype(f32).reshape(n * rows, cols)
        outs[8 + i][...] = (held - every).astype(bf16)


def solution(mesh):
    n, m = mesh.shape["fs"], mesh.shape["tp"]

    def body(
        latent,
        key_cot,
        value_cot,
        key_weight,
        value_weight,
        key_proj,
        value_proj,
        key_first,
        key_second,
        value_first,
        value_second,
    ):
        f32, bf16 = jnp.float32, jnp.bfloat16
        sds = jax.ShapeDtypeStruct
        tokens, width = latent.shape
        rows, cols = key_weight.shape
        rank = key_proj.shape[1]
        piece = 2 * rank // n
        dma = pltpu.SemaphoreType.DMA
        gathered, weights, squares = pl.pallas_call(
            functools.partial(exchange_kernel, n, m),
            out_shape=(
                sds((n, piece, cols), bf16),
                sds((n, 2, rows, cols), bf16),
                sds((n, 16, cols), f32),
            ),
            in_specs=[HBM] * 7,
            out_specs=(VMEM,) * 3,
            scratch_shapes=[
                pltpu.VMEM((CHUNKS, tokens, width // CHUNKS), bf16),
                pltpu.VMEM((2, tokens, cols), bf16),
                pltpu.VMEM((2 * cols, tokens), bf16),
                pltpu.VMEM((2, rows, cols), f32),
                pltpu.VMEM((2, width, rank), bf16),
                pltpu.VMEM((2 * rank, cols), bf16),
                pltpu.VMEM((n, piece, cols), bf16),
                pltpu.VMEM((m, 16, cols), f32),
                dma((6,)),
                dma((CHUNKS,)),
                dma((n,)),
                dma((n,)),
                dma((n,)),
                dma((n,)),
                dma((n,)),
                dma((n,)),
                dma((n,)),
                dma((n,)),
                dma((m,)),
                dma((m,)),
                dma((n,)),
                dma((n,)),
            ],
            compiler_params=pltpu.CompilerParams(
                collective_id=0, has_side_effects=True, vmem_limit_bytes=24 << 20
            ),
        )(latent, key_cot, value_cot, key_weight, value_weight, key_proj, value_proj)
        small = sds((rows, cols), f32)
        moment = sds((rank, cols), f32)
        copy = sds((n * rows, cols), bf16)
        return pl.pallas_call(
            functools.partial(update_kernel, n, float(rows * cols * n * m)),
            out_shape=(small,) * 4 + (moment,) * 4 + (copy,) * 2,
            in_specs=[VMEM] * 11,
            out_specs=(VMEM,) * 10,
            compiler_params=pltpu.CompilerParams(vmem_limit_bytes=24 << 20),
        )(
            gathered,
            weights,
            squares,
            key_weight,
            value_weight,
            key_proj,
            value_proj,
            key_first,
            key_second,
            value_first,
            value_second,
        )

    split, column = P("fs", "tp"), P(None, "tp")
    return jax.shard_map(
        body,
        mesh=mesh,
        in_specs=(P("fs", None),) + (split,) * 4 + (P(),) * 2 + (column,) * 4,
        out_specs=(split,) * 4 + (column,) * 6,
        check_vma=False,
    )
```

```python
import functools

import jax
import jax.numpy as jnp
from jax import lax
from jax.experimental import pallas as pl
from jax.experimental.pallas import tpu as pltpu
from jax.sharding import PartitionSpec as P

EPSILON = 1e-08
FIRST_DECAY = 0.7
SECOND_DECAY = 0.8
LEARN_RATE = 0.2
CHUNKS = 4
MESH = pl.DeviceIdType.MESH
HBM = pl.BlockSpec(memory_space=pltpu.MemorySpace.HBM)
VMEM = pl.BlockSpec(memory_space=pltpu.MemorySpace.VMEM)


def exchange_kernel(
    n,
    m,
    latent,
    key_cot,
    value_cot,
    key_weight,
    value_weight,
    key_proj,
    value_proj,
    key_first,
    key_second,
    value_first,
    value_second,
    gathered,
    weights,
    squares,
    weight_v,
    proj_v,
    moment_v,
    latent_v,
    cot_v,
    cot_t,
    partial,
    received,
    tp_squares,
    load_sem,
    latent_sem,
    rs_send,
    rs_recv,
    ag_send,
    ag_recv,
    w_send,
    w_recv,
    f_send,
    f_recv,
    t_send,
    t_recv,
    s_send,
    s_recv,
):
    me = lax.axis_index("fs")
    mine = lax.axis_index("tp")
    core = lax.rem(me, 2)
    partner = me + 1 - 2 * core
    half = n // 2
    tokens, width = latent.shape
    step = width // CHUNKS
    rank = key_proj.shape[1]
    cols = key_cot.shape[1]
    piece = partial.shape[0] // n
    f32, bf16 = jnp.float32, jnp.bfloat16

    loads = [
        pltpu.make_async_copy(src, dst, load_sem.at[i])
        for i, (src, dst) in enumerate(
            (
                (key_weight, weight_v.at[0]),
                (value_weight, weight_v.at[1]),
                (key_cot, cot_v.at[0]),
                (value_cot, cot_v.at[1]),
                (key_proj, proj_v.at[0]),
                (value_proj, proj_v.at[1]),
                (key_first, moment_v.at[0]),
                (key_second, moment_v.at[1]),
                (value_first, moment_v.at[2]),
                (value_second, moment_v.at[3]),
            )
        )
    ]
    streams = [
        pltpu.make_async_copy(
            latent.at[:, pl.ds(c * step, step)], latent_v.at[c], latent_sem.at[c]
        )
        for c in range(CHUNKS)
    ]
    for copy in loads[:4]:
        copy.start()
    streams[0].start()
    for copy in loads[4:6]:
        copy.start()
    for copy in streams[1:]:
        copy.start()
    for copy in loads[6:]:
        copy.start()

    barrier = pltpu.get_barrier_semaphore()
    for d in range(1, n):
        pl.semaphore_signal(
            barrier, inc=1, device_id={"fs": lax.rem(me + d, n)}, device_id_type=MESH
        )
    for d in range(1, m):
        pl.semaphore_signal(
            barrier, inc=1, device_id={"tp": lax.rem(mine + d, m)}, device_id_type=MESH
        )

    def send(src, dst, send_sem, recv_sem, where):
        copy = pltpu.make_async_remote_copy(
            src_ref=src,
            dst_ref=dst,
            send_sem=send_sem,
            recv_sem=recv_sem,
            device_id=where,
            device_id_type=MESH,
        )
        copy.start()
        return copy

    def arrived(ref, sem):
        pltpu.make_async_remote_copy(
            src_ref=ref,
            dst_ref=ref,
            send_sem=sem,
            recv_sem=sem,
            device_id={"fs": partner},
            device_id_type=MESH,
        ).wait_recv()

    chip = lax.div(me, 2)
    side = lax.div(chip, (half + 1) // 2)

    def far_first(k):
        down = half - 1 - k
        down = down - lax.div(chip - down + half, half)
        up = k + lax.div(k - chip + half, half)
        return down + side * (up - down)

    def peers():
        for k in range(half - 1):
            base = 2 * far_first(k)
            yield base + 1 - core
            yield base + core
        yield partner

    sent = []
    loads[0].wait()
    loads[1].wait()
    for i in range(2):
        w = weight_v[i]
        weights[me, i] = w.astype(bf16)
        tp_squares[mine, pl.ds(i, 1), :] = jnp.sum(w * w, axis=0, keepdims=True)
    loads[2].wait()
    loads[3].wait()
    for i in range(2):
        cot_t[pl.ds(i * cols, cols), :] = cot_v[i].T

    pl.semaphore_wait(barrier, n - 1 + m - 1)

    def send_weights(d):
        sent.append(
            send(
                weights.at[me],
                weights.at[me],
                w_send.at[d],
                w_recv.at[me],
                {"fs": 2 * far_first(d - 1) + core},
            )
        )

    for d in range(1, m):
        sent.append(
            send(
                tp_squares.at[mine],
                tp_squares.at[mine],
                t_send.at[d],
                t_recv.at[mine],
                {"tp": lax.rem(mine + d, m)},
            )
        )
    sent.append(
        send(
            weights.at[me], weights.at[me], f_send.at[0], f_recv.at[me], {"fs": partner}
        )
    )
    for d in range(1, half):
        send_weights(d)

    totals = [None, None]
    for c in range(CHUNKS):
        streams[c].wait()
        g = jnp.dot(cot_t[...], latent_v[c], preferred_element_type=f32).astype(bf16)
        if c == 0:
            loads[4].wait()
            loads[5].wait()
        for i in range(2):
            term = jnp.dot(
                g[i * cols : (i + 1) * cols],
                proj_v[i, pl.ds(c * step, step), :],
                preferred_element_type=f32,
            )
            totals[i] = term if totals[i] is None else totals[i] + term
    for i in range(2):
        partial[pl.ds(i * rank, rank), :] = totals[i].T.astype(bf16)

    for d in range(1, m):
        arrived(tp_squares.at[lax.rem(mine + d, m)], t_recv.at[lax.rem(mine + d, m)])
    squares[me] = jnp.sum(tp_squares[...], axis=0)

    for d, peer in enumerate(peers()):
        sent.append(
            send(
                partial.at[pl.ds(peer * piece, piece)],
                received.at[me],
                rs_send.at[d],
                rs_recv.at[me],
                {"fs": peer},
            )
        )
    received[me] = partial[pl.ds(pl.multiple_of(me * piece, piece), piece), :]
    for d in range(1, n):
        sent.append(
            send(
                squares.at[me],
                squares.at[me],
                s_send.at[d],
                s_recv.at[me],
                {"fs": lax.rem(me + d, n)},
            )
        )
    for d in range(1, n):
        peer = lax.rem(me + d, n)
        arrived(received.at[peer], rs_recv.at[peer])
    gathered[me] = jnp.sum(received[...].astype(f32), axis=0).astype(bf16)
    for d, peer in enumerate(peers()):
        sent.append(
            send(
                gathered.at[me],
                gathered.at[me],
                ag_send.at[d],
                ag_recv.at[me],
                {"fs": peer},
            )
        )
    for d in range(1, half):
        source = lax.rem(me + 2 * d, n)
        arrived(weights.at[source], w_recv.at[source])
        sent.append(
            send(
                weights.at[source],
                weights.at[source],
                f_send.at[d],
                f_recv.at[source],
                {"fs": partner},
            )
        )
    for d in range(half):
        source = lax.rem(partner + 2 * d, n)
        arrived(weights.at[source], f_recv.at[source])
    for d in range(1, n):
        peer = lax.rem(me + d, n)
        arrived(squares.at[peer], s_recv.at[peer])
    for d in range(1, n):
        peer = lax.rem(me + d, n)
        arrived(gathered.at[peer], ag_recv.at[peer])
    for copy in loads[6:]:
        copy.wait()
    for copy in sent:
        copy.wait_send()


def update_kernel(n, entries, *refs):
    gathered, weights, squares, weight_v, proj_v, moment_v = refs[:6]
    outs, stage, sems = refs[6:16], refs[16:26], refs[26]
    me = lax.axis_index("fs")
    f32, bf16 = jnp.float32, jnp.bfloat16
    parts = n // 2
    rows, cols = weight_v.shape[1:]
    rank = moment_v.shape[1]
    copies = [
        pltpu.make_async_copy(src, dst, sems.at[i])
        for i, (src, dst) in enumerate(zip(stage, outs))
    ]
    normalized = []
    for i in range(2):
        projected = (
            gathered[i * parts : (i + 1) * parts].astype(f32).reshape(rank, cols)
        )
        first_new = FIRST_DECAY * moment_v[2 * i] + (1.0 - FIRST_DECAY) * projected
        second_new = (
            SECOND_DECAY * moment_v[2 * i + 1]
            + (1.0 - SECOND_DECAY) * projected * projected
        )
        stage[4 + 2 * i][...] = first_new
        stage[5 + 2 * i][...] = second_new
        copies[4 + 2 * i].start()
        copies[5 + 2 * i].start()
        normalized.append((first_new / (jnp.sqrt(second_new) + EPSILON)).astype(bf16))
    tile = jnp.sum(squares[...], axis=0)
    for i in range(2):
        total = jnp.sum(tile[i : i + 1], keepdims=True)
        scale = LEARN_RATE * jnp.sqrt(total / entries)
        every = scale * jnp.dot(proj_v[i], normalized[i], preferred_element_type=f32)
        held = weights[:, i].astype(f32).reshape(n * rows, cols)
        stage[8 + i][...] = (held - every).astype(bf16)
        copies[8 + i].start()
        own = proj_v[i, pl.ds(pl.multiple_of(me * rows, rows), rows), :]
        own_step = scale * jnp.dot(own, normalized[i], preferred_element_type=f32)
        stage[2 + i][...] = own_step
        stage[i][...] = weight_v[i] - own_step
        copies[2 + i].start()
        copies[i].start()
    for copy in copies:
        copy.wait()


def solution(mesh):
    n, m = mesh.shape["fs"], mesh.shape["tp"]

    def body(
        latent,
        key_cot,
        value_cot,
        key_weight,
        value_weight,
        key_proj,
        value_proj,
        key_first,
        key_second,
        value_first,
        value_second,
    ):
        f32, bf16 = jnp.float32, jnp.bfloat16
        sds = jax.ShapeDtypeStruct
        tokens, width = latent.shape
        rows, cols = key_weight.shape
        rank = key_proj.shape[1]
        piece = 2 * rank // n
        dma = pltpu.SemaphoreType.DMA
        held = pl.pallas_call(
            functools.partial(exchange_kernel, n, m),
            out_shape=(
                sds((n, piece, cols), bf16),
                sds((n, 2, rows, cols), bf16),
                sds((n, 2, cols), f32),
                sds((2, rows, cols), f32),
                sds((2, width, rank), bf16),
                sds((4, rank, cols), f32),
            ),
            in_specs=[HBM] * 11,
            out_specs=(VMEM,) * 6,
            scratch_shapes=[
                pltpu.VMEM((CHUNKS, tokens, width // CHUNKS), bf16),
                pltpu.VMEM((2, tokens, cols), bf16),
                pltpu.VMEM((2 * cols, tokens), bf16),
                pltpu.VMEM((2 * rank, cols), bf16),
                pltpu.VMEM((n, piece, cols), bf16),
                pltpu.VMEM((m, 2, cols), f32),
                dma((10,)),
                dma((CHUNKS,)),
                dma((n,)),
                dma((n,)),
                dma((n,)),
                dma((n,)),
                dma((n,)),
                dma((n,)),
                dma((n,)),
                dma((n,)),
                dma((m,)),
                dma((m,)),
                dma((n,)),
                dma((n,)),
            ],
            compiler_params=pltpu.CompilerParams(
                collective_id=0, has_side_effects=True, vmem_limit_bytes=24 << 20
            ),
        )(
            *(
                pltpu.with_memory_space_constraint(x, pltpu.MemorySpace.HBM)
                for x in (
                    latent,
                    key_cot,
                    value_cot,
                    key_weight,
                    value_weight,
                    key_proj,
                    value_proj,
                    key_first,
                    key_second,
                    value_first,
                    value_second,
                )
            )
        )
        small = sds((rows, cols), f32)
        moment = sds((rank, cols), f32)
        copy = sds((n * rows, cols), bf16)
        return pl.pallas_call(
            functools.partial(update_kernel, n, float(rows * cols * n * m)),
            out_shape=(small,) * 4 + (moment,) * 4 + (copy,) * 2,
            in_specs=[VMEM] * 6,
            out_specs=(HBM,) * 10,
            scratch_shapes=[pltpu.VMEM((rows, cols), f32)] * 4
            + [pltpu.VMEM((rank, cols), f32)] * 4
            + [pltpu.VMEM((n * rows, cols), bf16)] * 2
            + [dma((10,))],
            compiler_params=pltpu.CompilerParams(vmem_limit_bytes=24 << 20),
        )(*held)

    split, column = P("fs", "tp"), P(None, "tp")
    return jax.shard_map(
        body,
        mesh=mesh,
        in_specs=(P("fs", None),) + (split,) * 4 + (P(),) * 2 + (column,) * 4,
        out_specs=(split,) * 4 + (column,) * 6,
        check_vma=False,
    )
```
